32 devices in a mesh: ep: 8 (over z, x), tp: 4 (over y, core).
Axes of the slice: x: 2, y: 2, z: 4, core: 2. Of those that a mesh axis runs over, the one named last changes fastest.
Arguments:
- mix_in: bfloat16 [1024, 2048], P('ep'), may hold values from -6 to 6
- mix_gain: float32 [2048], replicated, may hold values from 0.1 to 1.9
- query_weight: bfloat16 [2048, 3072], P(None, 'tp'), may hold values from -0.125 to 0.125
- latent_weight: bfloat16 [2048, 512], replicated, may hold values from -0.125 to 0.125
- rotary_weight: bfloat16 [2048, 64], replicated, may hold values from -0.125 to 0.125
- latent_gain: float32 [512], replicated, may hold values from 0.1 to 1.9
- key_weight: bfloat16 [512, 2048], P(None, 'tp'), may hold values from -0.25 to 0.25
- value_weight: bfloat16 [512, 2048], P(None, 'tp'), may hold values from -0.25 to 0.25
- output_weight: bfloat16 [2048, 2048], P('tp'), may hold values from -0.125 to 0.125
- out_gain: float32 [2048], replicated, may hold values from 0.1 to 1.9
- ffn_in: bfloat16 [1024, 2048], P('ep'), may hold values from -6 to 6
- ffn_gain: float32 [2048], replicated, may hold values from 0.1 to 1.9
- gate_weight: bfloat16 [8, 2048, 1024], P('ep', None, 'tp'), may hold values from -0.375 to 0.375
- up_weight: bfloat16 [8, 2048, 1024], P('ep', None, 'tp'), may hold values from -0.375 to 0.375
- down_weight: bfloat16 [8, 1024, 2048], P('ep', 'tp'), may hold values from -0.046875 to 0.046875
- routes: int32 [1024, 4], P('ep'), may hold values from 0 to 7, all different within a row; in each aligned block of 32 rows (0 to 31, 32 to 63, ...) at most 32 rows name the same one
- route_scores: float32 [1024, 4], P('ep'), may hold values from -6 to 6
Outputs:
- mixed: bfloat16 [1024, 2048], P(('ep', 'tp'))
- moe_out: bfloat16 [1024, 2048], P(('ep', 'tp'))
The draws below stay inside these ranges and needn't reach their ends.
Inputs may be any that keep to these rules, and one draw needn't show every extreme that they name: `routes`: each row names 4 different experts; in each aligned block of 32 rows no expert is named by more than 32 rows, a bound that some blocks reach.
All inputs are finite; a program needn't handle non-finite values.
Results may differ from the reference program's by a relative error of at most 0.014.
Values may be sent and summed in bfloat16 or wider, within the bound.
A program may use at most 192 MiB of HBM per device.

```python
import math
import jax
import jax.numpy as jnp
import numpy as np
from jax import lax

D = 2048
HEADS = 16
NOPE = 128
ROPE = 64
VD = 128
KVR = 512
FF = 1024
TOP = 4
EXPERTS = 8
TOKENS_A = 1024
TOKENS_B = 1024
QB = 32
MOST = 32
N_TP = 4


def steps_of(own_key, shape, pieces, least, high):
    factor_of = 1.0
    for position, blocks in pieces:
        heights = jax.random.uniform(jax.random.fold_in(jax.random.fold_in(own_key, 6), position), (blocks,), jnp.float32, least / len(pieces), high / len(pieces))
        factor_of = factor_of * jnp.repeat(jnp.exp(heights), shape[position] // blocks).reshape((-1,) + (1,) * (len(shape) - 1 - position))
    return factor_of


def assign_block(key, own, number, rows, count, top, bound, slope):
    ranking = jax.random.permutation(key, count)
    crowded, usual = portions_of(count, rows * top, bound, slope, True), portions_of(count, rows * top, bound, slope, False)
    places = jnp.arange(count)

    def named(lengths, turn):
        used = int((lengths > 0).sum())
        fixed = max(1, used // 4)
        moved = fixed + (places - fixed + turn * (used - fixed)) % max(1, count - fixed)
        return jnp.zeros((count,), jnp.int32).at[ranking[jnp.where(places < fixed, places, moved)]].set(jnp.asarray(lengths, jnp.int32))

    lengths = jnp.where(number % 4 == 0, named(crowded, number // 4), named(usual, number - number // 4 - 1))
    mixed = jax.random.permutation(jax.random.fold_in(own, 3), count)
    source_of, taker = mixed[0:count // 2 * 2:2], mixed[1:count // 2 * 2:2]
    room = jnp.minimum(lengths[source_of] - 1, bound - lengths[taker]) // 2
    room = jnp.where((source_of == ranking[0]) | (taker == ranking[0]) | (lengths[taker] == 0), 0, jnp.maximum(room, 0))
    moved = jax.random.randint(jax.random.fold_in(own, 4), (count // 2,), 0, 1 << 20) % (room + 1)
    lengths = lengths.at[source_of].add(-moved).at[taker].add(moved)
    items = jnp.searchsorted(jnp.cumsum(lengths), jnp.arange(rows * top), side="right").astype(jnp.int32)
    table = items.reshape(top, rows).T
    table = table[jax.random.permutation(jax.random.fold_in(own, 1), rows)]
    turn = jax.random.randint(jax.random.fold_in(own, 2), (rows, 1), 0, top)
    return jnp.take_along_axis(table, (jnp.arange(top)[None, :] + turn) % top, axis=1)


def portions_of(count, total, most, lean, full):
    portions = [(1 << 20) // math.isqrt(grade ** lean) + 1 for grade in range(1, count + 1)]
    largest = most if full else min(most, max(-(-total // count), total * portions[0] // sum(portions)))
    least = 1 if total - largest >= count - 1 else 0
    holding, rest = [largest] + [least] * (count - 1), total - largest - least * (count - 1)
    while rest > 0:
        movable = [i for i in range(1, count) if holding[i] < largest] or [i for i in range(1, count) if holding[i] < most]
        mass, budget = sum([portions[i] for i in movable]), rest
        for i in movable:
            more = min(most - holding[i], max(1, budget * portions[i] // mass), rest)
            holding[i] = holding[i] + more
            rest = rest - more
    return np.array(holding)


def noise(own_key, dims, deviation, limit, split=(), kind=jnp.bfloat16):
    gain = steps_of(own_key, dims, split, -0.22, 0.18) if split else 1.0
    drawn = jax.random.normal(own_key, dims, jnp.float32) * deviation * gain
    return jnp.minimum(jnp.maximum(drawn, -limit), limit).astype(kind)


def setup_inputs(seed: int = 0) -> dict:
    key_list = jax.random.split(jax.random.key(seed), 18)
    mix_in = noise(key_list[0], (TOKENS_A, D), 1.0, 6.0, ((0, 8),))
    mix_gain = jnp.clip(1.0 + 0.18 * jax.random.normal(key_list[1], (D,), jnp.float32), 0.1, 1.9)
    query_weight = noise(key_list[2], (D, HEADS * (NOPE + ROPE)), D ** -0.5, 0.125, ((1, 4),))
    latent_weight = noise(key_list[3], (D, KVR), D ** -0.5, 0.125)
    rotary_weight = noise(key_list[4], (D, ROPE), D ** -0.5, 0.125)
    latent_gain = jnp.clip(1.0 + 0.18 * jax.random.normal(key_list[5], (KVR,), jnp.float32), 0.1, 1.9)
    key_weight = noise(key_list[6], (KVR, HEADS * NOPE), KVR ** -0.5, 0.25, ((1, 4),))
    value_weight = noise(key_list[7], (KVR, HEADS * VD), KVR ** -0.5, 0.25, ((1, 4),))
    output_weight = noise(key_list[8], (HEADS * VD, D), (HEADS * VD) ** -0.5, 0.125, ((0, 4),))
    out_gain = jnp.clip(1.0 + 0.18 * jax.random.normal(key_list[9], (D,), jnp.float32), 0.1, 1.9)
    ffn_in = noise(key_list[10], (TOKENS_B, D), 1.0, 6.0, ((0, 8),))
    ffn_gain = jnp.clip(1.0 + 0.18 * jax.random.normal(key_list[11], (D,), jnp.float32), 0.1, 1.9)
    gate_weight = noise(key_list[12], (EXPERTS, D, FF), (D // 8) ** -0.5, 0.375, ((0, 8), (2, 4)))
    up_weight = noise(key_list[13], (EXPERTS, D, FF), (D // 8) ** -0.5, 0.375, ((0, 8), (2, 4)))
    down_weight = noise(key_list[14], (EXPERTS, FF, D), (FF * 16) ** -0.5, 0.046875, ((0, 8), (1, 4)))
    routes_keys = jax.random.split(jax.random.fold_in(key_list[15], 1), TOKENS_B // QB)
    routes_turns = jax.random.permutation(jax.random.fold_in(key_list[15], 3), TOKENS_B // QB)
    routes = jax.vmap(lambda own, number: assign_block(jax.random.fold_in(key_list[15], 2), own, number, QB, EXPERTS, TOP, MOST, 2))(routes_keys, routes_turns).reshape((TOKENS_B, TOP))
    route_scores = noise(key_list[16], (TOKENS_B, TOP), 1.0, 6.0, ((0, 8),), jnp.float32)
    return dict(mix_in=mix_in, mix_gain=mix_gain, query_weight=query_weight, latent_weight=latent_weight, rotary_weight=rotary_weight, latent_gain=latent_gain, key_weight=key_weight, value_weight=value_weight, output_weight=output_weight, out_gain=out_gain, ffn_in=ffn_in, ffn_gain=ffn_gain, gate_weight=gate_weight, up_weight=up_weight, down_weight=down_weight, routes=routes, route_scores=route_scores)


norm_eps = 1e-06
clamp_limit = 7.0
gate_slope = 1.702
rope_base = 10000.0

def rms_rows(rows_in, scales):
    mean_square = lax.optimization_barrier(jnp.mean(rows_in * rows_in, axis=-1, keepdims=True))
    return rows_in * lax.rsqrt(mean_square + norm_eps) * scales.astype(jnp.float32)

def angle_tables(positions):
    inverse = rope_base ** (-jnp.arange(0, ROPE, 2).astype(jnp.float32) / ROPE)
    angle_rows = positions.astype(jnp.float32)[:, None] * inverse[None, :]
    return (jnp.cos(angle_rows), jnp.sin(angle_rows))

def rotate_last(vectors, cosine, sine_rows):
    half_rope = vectors.shape[-1] // 2
    upper_half = vectors[..., :half_rope]
    lower_half = vectors[..., half_rope:]
    return jnp.concatenate([upper_half * cosine - lower_half * sine_rows, lower_half * cosine + upper_half * sine_rows], axis=-1)

def clamped_unit(gate_part, linear):
    gate_part = jnp.minimum(gate_part, clamp_limit)
    linear = jnp.clip(linear, -clamp_limit, clamp_limit)
    return gate_part * jax.nn.sigmoid(gate_slope * gate_part) * (linear + 1.0)

def rounded(vectors):
    return lax.optimization_barrier(vectors.astype(jnp.bfloat16)).astype(jnp.float32)

def mixer_half(mix_in, mix_gain, query_weight, latent_weight, rotary_weight, latent_gain, key_weight, value_weight, output_weight, out_gain):
    length = mix_in.shape[0]
    normed = rms_rows(mix_in.astype(jnp.float32), mix_gain).astype(jnp.bfloat16)
    positions = jnp.arange(length, dtype=jnp.int32)
    cosine, sine_rows = angle_tables(positions)
    queries = jnp.dot(normed, query_weight, preferred_element_type=jnp.float32).reshape(length, HEADS, NOPE + ROPE)
    query_plain = queries[..., :NOPE].astype(jnp.bfloat16)
    query_turn = rotate_last(queries[..., NOPE:], cosine[:, None, :], sine_rows[:, None, :]).astype(jnp.bfloat16)
    latent = rms_rows(jnp.dot(normed, latent_weight, preferred_element_type=jnp.float32), latent_gain).astype(jnp.bfloat16)
    rotary_key = rotate_last(jnp.dot(normed, rotary_weight, preferred_element_type=jnp.float32), cosine, sine_rows).astype(jnp.bfloat16)
    key_rows = jnp.dot(latent, key_weight, preferred_element_type=jnp.float32).astype(jnp.bfloat16)
    key_rows = key_rows.reshape(length, HEADS, NOPE).astype(jnp.float32)
    value_rows = jnp.dot(latent, value_weight, preferred_element_type=jnp.float32).astype(jnp.bfloat16)
    value_rows = value_rows.reshape(length, HEADS, VD).astype(jnp.float32)
    rotary_wide = rotary_key.astype(jnp.float32)
    score_scale = (NOPE + ROPE) ** (-0.5)
    block_rows = math.gcd(length, 256)
    block_count = length // block_rows

    def attend(block_index):
        start_row = block_index * block_rows
        plain_block = lax.dynamic_slice_in_dim(query_plain, start_row, block_rows, 0).astype(jnp.float32)
        turn_block = lax.dynamic_slice_in_dim(query_turn, start_row, block_rows, 0).astype(jnp.float32)
        scores = jnp.einsum('ihd,jhd->hij', plain_block, key_rows)
        scores = scores + jnp.einsum('ihd,jd->hij', turn_block, rotary_wide)
        query_places = start_row + jnp.arange(block_rows, dtype=jnp.int32)
        allowed = positions[None, :] <= query_places[:, None]
        weights = jnp.where(allowed[None], jnp.exp(scores * score_scale), 0.0)
        totals = lax.optimization_barrier(jnp.sum(weights, axis=-1))
        weighted = jnp.einsum('hij,jhd->hid', rounded(weights), value_rows)
        return (weighted / totals[..., None]).astype(jnp.bfloat16)
    attended = lax.map(attend, jnp.arange(block_count))
    attended = attended.transpose(0, 2, 1, 3).reshape(length, HEADS, VD)
    group_heads = HEADS // N_TP
    projected = jnp.zeros((length, D), jnp.float32)
    for group in range(N_TP):
        head_block = attended[:, group * group_heads:(group + 1) * group_heads, :].reshape(length, group_heads * VD)
        weight_rows = output_weight[group * group_heads * VD:(group + 1) * group_heads * VD]
        projected = projected + rounded(jnp.dot(head_block, weight_rows, preferred_element_type=jnp.float32))
    return rms_rows(projected, out_gain).astype(jnp.bfloat16)

def expert_half(ffn_in, ffn_gain, gate_weight, up_weight, down_weight, routes, route_scores):
    row_count = ffn_in.shape[0]
    normed = rms_rows(ffn_in.astype(jnp.float32), ffn_gain).astype(jnp.bfloat16)
    padded = jnp.concatenate([normed, jnp.zeros((1, D), jnp.bfloat16)], axis=0)
    gate_share = jax.nn.softmax(route_scores.astype(jnp.float32), axis=-1).reshape(-1)
    gate_share = jnp.concatenate([gate_share, jnp.zeros((1,), jnp.float32)], axis=0)
    flat_routes = routes.reshape(-1)
    assignment_count = flat_routes.shape[0]
    capacity_all = MOST * (row_count // QB)
    unit_group = FF // N_TP

    def one_expert(totals, expert):
        matches = flat_routes == expert
        slot_rank = jnp.cumsum(matches.astype(jnp.int32)) - 1
        destination = jnp.where(matches, slot_rank, capacity_all).astype(jnp.int32)
        slot_of = jnp.full((capacity_all + 1,), assignment_count, jnp.int32)
        slot_of = slot_of.at[destination].set(jnp.arange(assignment_count, dtype=jnp.int32))[:capacity_all]
        token_of = slot_of // TOP
        gathered = padded[token_of]
        gate_part = jnp.dot(gathered, gate_weight[expert], preferred_element_type=jnp.float32)
        up_part = jnp.dot(gathered, up_weight[expert], preferred_element_type=jnp.float32)
        hidden = clamped_unit(gate_part, up_part).astype(jnp.bfloat16)
        expert_sum = jnp.zeros((capacity_all, D), jnp.float32)
        for group in range(N_TP):
            expert_sum = expert_sum + rounded(jnp.dot(hidden[:, group * unit_group:(group + 1) * unit_group], down_weight[expert][group * unit_group:(group + 1) * unit_group], preferred_element_type=jnp.float32))
        weighted = rounded(expert_sum) * gate_share[slot_of][:, None]
        totals = totals.at[token_of].add(weighted, mode='drop')
        return (totals, None)
    totals, _ = lax.scan(one_expert, jnp.zeros((row_count, D), jnp.float32), jnp.arange(EXPERTS, dtype=jnp.int32))
    return totals.astype(jnp.bfloat16)

def reference(mix_in, mix_gain, query_weight, latent_weight, rotary_weight, latent_gain, key_weight, value_weight, output_weight, out_gain, ffn_in, ffn_gain, gate_weight, up_weight, down_weight, routes, route_scores):
    mixed = mixer_half(mix_in, mix_gain, query_weight, latent_weight, rotary_weight, latent_gain, key_weight, value_weight, output_weight, out_gain)
    moe_out = expert_half(ffn_in, ffn_gain, gate_weight, up_weight, down_weight, routes, route_scores)
    return (mixed, moe_out)
```

```python
import jax
import jax.numpy as jnp
import functools
from jax import lax
from jax.experimental import pallas as pl
from jax.experimental.pallas import tpu as pltpu
from jax.sharding import PartitionSpec as P

NOPE = 128
ROPE = 64
VD = 128


norm_eps = 1e-06
clamp_limit = 7.0
gate_slope = 1.702
rope_base = 10000.0


def rms_rows(rows_in, scales):
    mean_square = jnp.mean(rows_in * rows_in, axis=-1, keepdims=True)
    return rows_in * lax.rsqrt(mean_square + norm_eps) * scales


def rms_columns(columns, scales):
    mean_square = jnp.mean(columns * columns, axis=0, keepdims=True)
    return columns * lax.rsqrt(mean_square + norm_eps) * scales[:, None]


def turn_table(positions):
    inverse = rope_base ** (-jnp.arange(0, ROPE, 2).astype(jnp.float32) / ROPE)
    angle_rows = inverse[:, None] * positions.astype(jnp.float32)[None, :]
    return (jnp.cos(angle_rows), jnp.sin(angle_rows))


def clamped_unit(gate_part, linear):
    gate_part = jnp.minimum(gate_part, clamp_limit)
    linear = jnp.clip(linear, -clamp_limit, clamp_limit)
    return gate_part * jax.nn.sigmoid(gate_slope * gate_part) * (linear + 1.0)


def keep_state(running):
    return running


def local(
    mix_in,
    mix_gain,
    query_weight,
    latent_weight,
    rotary_weight,
    latent_gain,
    key_weight,
    value_weight,
    output_weight,
    out_gain,
    ffn_in,
    ffn_gain,
    gate_weight,
    up_weight,
    down_weight,
    routes,
    route_scores,
):
    row_count = mix_in.shape[0]
    first_row = lax.axis_index("ep") * row_count
    last_row = first_row + row_count - 1
    positions = first_row + jnp.arange(row_count, dtype=jnp.int32)
    normed = rms_rows(mix_in.astype(jnp.float32), mix_gain).astype(jnp.bfloat16)
    head_count = query_weight.shape[1] // (NOPE + ROPE)
    half_rope = ROPE // 2
    cosine, sine_rows = turn_table(positions)
    queries = jnp.dot(normed, query_weight, preferred_element_type=jnp.float32).reshape(
        row_count, head_count, NOPE + ROPE
    )
    query_plain = queries[..., :NOPE].astype(jnp.bfloat16)
    query_cos = cosine.T[:, None, :]
    query_sin = sine_rows.T[:, None, :]
    query_upper = queries[..., NOPE : NOPE + half_rope]
    query_lower = queries[..., NOPE + half_rope :]
    query_turn = jnp.concatenate(
        [
            query_upper * query_cos - query_lower * query_sin,
            query_lower * query_cos + query_upper * query_sin,
        ],
        axis=-1,
    ).astype(jnp.bfloat16)
    across = (((0,), (1,)), ((), ()))
    latent = rms_columns(
        lax.dot_general(latent_weight, normed, across, preferred_element_type=jnp.float32),
        latent_gain,
    ).astype(jnp.bfloat16)
    rot_raw = lax.dot_general(rotary_weight, normed, across, preferred_element_type=jnp.float32)
    rotary_key = jnp.concatenate(
        [
            rot_raw[:half_rope] * cosine - rot_raw[half_rope:] * sine_rows,
            rot_raw[half_rope:] * cosine + rot_raw[:half_rope] * sine_rows,
        ],
        axis=0,
    ).astype(jnp.bfloat16)
    score_scale = (NOPE + ROPE) ** (-0.5)
    contract_first = (((0,), (0,)), ((), ()))

    def expand(latent_block):
        key_block = lax.dot_general(
            key_weight, latent_block, contract_first, preferred_element_type=jnp.float32
        ).astype(jnp.bfloat16)
        value_block = lax.dot_general(
            value_weight, latent_block, contract_first, preferred_element_type=jnp.float32
        ).astype(jnp.bfloat16)
        return (key_block, value_block)

    def attend(key_block, value_block, turn_block):
        key_count = key_block.shape[1]
        key_block = key_block.reshape(head_count, NOPE, key_count)
        value_block = value_block.reshape(head_count, VD, key_count)
        scores = jnp.einsum(
            "ihd,hdj->hij", query_plain, key_block, preferred_element_type=jnp.float32
        )
        scores = scores + jnp.einsum(
            "ihd,dj->hij", query_turn, turn_block, preferred_element_type=jnp.float32
        )
        key_places = jnp.arange(key_count, dtype=jnp.int32)
        allowed = key_places[None, :] <= positions[:, None]
        weights = jnp.where(allowed[None], jnp.exp(scores * score_scale), 0.0)
        weighted = jnp.einsum(
            "hij,hdj->hid",
            weights.astype(jnp.bfloat16),
            value_block,
            preferred_element_type=jnp.float32,
        )
        return (jnp.sum(weights, axis=-1), weighted)

    initial = (
        jnp.zeros((head_count, row_count), jnp.float32),
        jnp.zeros((head_count, row_count, VD), jnp.float32),
    )
    shard_piece = (
        lax.all_gather(latent, "ep", axis=1, tiled=True),
        lax.all_gather(rotary_key, "ep", axis=1, tiled=True),
    )

    def compute_piece(running):
        key_block, value_block = expand(shard_piece[0])
        return attend(key_block, value_block, shard_piece[1])

    totals, weighted = lax.cond(jnp.int32(0) > last_row, keep_state, compute_piece, initial)
    attended = (weighted / totals[..., None]).astype(jnp.bfloat16)
    mixing = output_weight.reshape(head_count, VD, output_weight.shape[1])
    partial_value = jnp.einsum("hid,hde->ie", attended, mixing, preferred_element_type=jnp.float32)
    projected = lax.psum_scatter(
        lax.optimization_barrier(partial_value.astype(jnp.bfloat16))
        .astype(jnp.float32)
        .astype(jnp.bfloat16),
        "tp",
        scatter_dimension=0,
        tiled=True,
    ).astype(jnp.float32)
    mixed = rms_rows(projected, out_gain).astype(jnp.bfloat16)
    tokens = ffn_in.shape[0]
    part_count = lax.axis_size("tp")
    quarter_rows = tokens // part_count
    experts = lax.axis_size("ep")
    choose = routes.shape[1]
    capacity = max(2, 2 * quarter_rows * choose // experts)
    slot_count = capacity * part_count
    tp_index = lax.axis_index("tp")
    normed_b = rms_rows(ffn_in.astype(jnp.float32), ffn_gain).astype(jnp.bfloat16)
    padded = jnp.concatenate([normed_b, jnp.zeros((1, normed_b.shape[1]), jnp.bfloat16)], axis=0)
    gate_share = jax.nn.softmax(route_scores, axis=-1)
    grouped = routes.reshape(part_count, quarter_rows * choose)
    onehot = (grouped[:, :, None] == jnp.arange(experts, dtype=jnp.int32)[None, None, :]).astype(
        jnp.int32
    )
    slot_rank = jnp.sum((jnp.cumsum(onehot, axis=1) - 1) * onehot, axis=2)
    slot_index = jnp.arange(part_count, dtype=jnp.int32)[:, None] * capacity + slot_rank
    place_index = (slot_index * experts + grouped).reshape(-1)
    owners = jnp.arange(tokens * choose, dtype=jnp.int32) // choose
    slot_token = jnp.full((slot_count * experts,), tokens, jnp.int32).at[place_index].set(owners)
    unit_count = gate_weight.shape[2]
    chosen = lax.dynamic_slice_in_dim(
        slot_token, tp_index * capacity * experts, capacity * experts, 0
    )
    outgoing = padded[chosen].reshape(capacity, experts, -1)
    arrived = lax.all_to_all(outgoing, "ep", split_axis=1, concat_axis=1, tiled=True)
    row_block = lax.all_gather(arrived, "tp", axis=0, tiled=True)
    block_slots = row_block.shape[0]
    flat_rows = row_block.reshape(-1, row_block.shape[2])
    gate_part = jnp.dot(flat_rows, gate_weight[0], preferred_element_type=jnp.float32)
    up_part = jnp.dot(flat_rows, up_weight[0], preferred_element_type=jnp.float32)
    hidden = (
        clamped_unit(gate_part, up_part).astype(jnp.bfloat16).reshape(block_slots, -1, unit_count)
    )
    sources = hidden.shape[1]
    hidden_flat = hidden.reshape(slot_count * sources, unit_count)
    partial_value = jnp.dot(hidden_flat, down_weight[0], preferred_element_type=jnp.float32)
    result = lax.psum_scatter(
        lax.optimization_barrier(partial_value.astype(jnp.bfloat16))
        .astype(jnp.float32)
        .astype(jnp.bfloat16),
        "tp",
        scatter_dimension=0,
        tiled=True,
    )
    result = result.reshape(capacity, sources, -1)
    returned = lax.all_to_all(result, "ep", split_axis=1, concat_axis=1, tiled=True)
    back_rows = returned.reshape(capacity * experts, -1)
    own_rank = lax.dynamic_index_in_dim(slot_rank, tp_index, 0, keepdims=False)
    own_expert = lax.dynamic_index_in_dim(grouped, tp_index, 0, keepdims=False)
    picked = (
        back_rows[own_rank * experts + own_expert]
        .astype(jnp.float32)
        .reshape(quarter_rows, choose, -1)
    )
    own_gates = lax.dynamic_slice_in_dim(gate_share, tp_index * quarter_rows, quarter_rows, 0)
    moe_out = jnp.sum(picked * own_gates[:, :, None], axis=1).astype(jnp.bfloat16)
    return (mixed, moe_out)


MESH = pl.DeviceIdType.MESH


def flip(value, bits):
    bit = 1
    while bit <= bits:
        if bits & bit:
            value = value + bit - 2 * bit * ((value // bit) % 2)
        bit *= 2
    return value


def here():
    ep, tp = lax.axis_index("ep"), lax.axis_index("tp")
    return ep // 2, ep % 2, tp // 2, tp % 2


def place(z, x, y, core):
    return {"ep": z * 2 + x, "tp": y * 2 + core}


def greet(partners):
    barrier = pltpu.get_barrier_semaphore()
    for partner in partners:
        pl.semaphore_signal(barrier, inc=1, device_id=partner, device_id_type=MESH)
    pl.semaphore_wait(barrier, len(partners))


def gather_kernel(depth, row_ref, side_ref, rows_out, side_out, send_sem, recv_sem):
    z, x, y, core = here()
    x_next, y_next, twin = place(z, 1 - x, y, core), place(z, x, 1 - y, core), place(z, x, y, 1 - core)
    columns = [place(flip(z, d), x, y, core) for d in range(1, depth)]
    greet(columns + [x_next, y_next, twin])
    started = []

    def copies(origin, target, own):
        e, t = origin["ep"], origin["tp"]
        number = len(started)
        return [
            pltpu.make_async_remote_copy(
                src_ref=mine if own else out.at[e, t],
                dst_ref=out.at[e, t],
                send_sem=send_sem.at[a, number],
                recv_sem=recv_sem.at[a, e, t],
                device_id=target,
                device_id_type=MESH,
            )
            for a, (mine, out) in enumerate(((side_ref, side_out), (row_ref, rows_out)))
        ]

    def send(origin, target, own=False):
        pair = copies(origin, target, own)
        for copy in pair:
            copy.start()
        started.append(pair)

    def arrive(origin):
        for copy in copies(origin, twin, False):
            copy.wait_recv()

    me = place(z, x, y, core)
    for target in columns + [x_next, y_next, twin]:
        send(me, target, True)
    rows_out[me["ep"], me["tp"]] = row_ref[...]
    side_out[me["ep"], me["tp"]] = side_ref[...]

    def square(d):
        at = flip(z, d)
        from_x, from_y = place(at, 1 - x, y, core), place(at, x, 1 - y, core)
        arrive(from_x)
        if d % 2 == 0:
            send(from_x, y_next)
        send(from_x, twin)
        arrive(from_y)
        if d % 2 == 1:
            send(from_y, x_next)
        send(from_y, twin)

    for d in range(1, depth):
        origin = place(flip(z, d), x, y, core)
        arrive(origin)
        for target in (x_next, y_next, twin):
            send(origin, target)
        square(d - 1)
    square(depth - 1)
    for d in range(depth):
        origin = place(flip(z, d), 1 - x, 1 - y, core)
        arrive(origin)
        send(origin, twin)
    for d in range(depth):
        for a in (x, 1 - x):
            for b in (y, 1 - y):
                arrive(place(flip(z, d), a, b, 1 - core))
    for pair in started:
        for copy in pair:
            copy.wait_send()


def gather_blocks(rows, side, experts, parts):
    depth = experts // 2
    sends = depth + 2 + 3 * (depth - 1) + 3 * depth + depth
    whole = [jax.ShapeDtypeStruct((experts, parts) + a.shape, a.dtype) for a in (rows, side)]
    vmem = pl.BlockSpec(memory_space=pltpu.VMEM)
    return pl.pallas_call(
        functools.partial(gather_kernel, depth),
        out_shape=whole,
        in_specs=[vmem] * 2,
        out_specs=[vmem] * 2,
        scratch_shapes=[
            pltpu.SemaphoreType.DMA((2, sends)),
            pltpu.SemaphoreType.DMA((2, experts, parts)),
        ],
        compiler_params=pltpu.CompilerParams(
            collective_id=0, has_side_effects=True, vmem_limit_bytes=48 * 1024 * 1024
        ),
        name="gather_blocks",
    )(rows, side)


def reduce_kernel(
    depth, part_ref, heads_ref, gain_ref, mixed_ref, moe_ref,
    work, twin_in, hop_in, direct_in, relay_in, column_in,
    heads_work, heads_twin, heads_in, send_sem, twin_sem, square_sem, column_sem, heads_sem,
):
    z, x, y, core = here()
    x_next, y_next, twin = place(z, 1 - x, y, core), place(z, x, 1 - y, core), place(z, x, y, 1 - core)
    columns = [place(flip(z, d), x, y, core) for d in range(1, depth)]
    greet(columns + [x_next, y_next, twin])
    started = []

    def make(src, dst, sem, target):
        return pltpu.make_async_remote_copy(
            src_ref=src, dst_ref=dst, send_sem=send_sem.at[len(started)], recv_sem=sem,
            device_id=target, device_id_type=MESH,
        )

    def send(src, dst, sem, target):
        copy = make(src, dst, sem, target)
        copy.start()
        started.append(copy)

    def arrive(dst, sem):
        make(dst, dst, sem, twin).wait_recv()

    def mine(d, a, b):
        return part_ref[flip(z, d) * 2 + flip(x, a), flip(y, b) * 2 + core].astype(jnp.float32)

    order = list(range(1, depth)) + [0]
    for b in (1, 0):
        send(heads_ref.at[flip(y, b) * 2 + 1 - core], heads_twin.at[b], heads_sem.at[b], twin)
    turns = [(1, 1), (1, 0), (0, 1), (0, 0)]
    for d in order:
        for a, b in turns:
            e, t = flip(z, d) * 2 + flip(x, a), flip(y, b) * 2 + 1 - core
            send(part_ref.at[e, t], twin_in.at[d, a, b], twin_sem.at[d, a, b], twin)

    arrive(heads_twin.at[1], heads_sem.at[1])
    heads_work[...] = (
        heads_ref[(1 - y) * 2 + core].astype(jnp.float32) + heads_twin[1].astype(jnp.float32)
    ).astype(jnp.bfloat16)
    send(heads_work, heads_in, heads_sem.at[2], y_next)

    def paired(d, a, b):
        arrive(twin_in.at[d, a, b], twin_sem.at[d, a, b])
        return mine(d, a, b) + twin_in[d, a, b].astype(jnp.float32)

    for d in order:
        work[d, 1, 1] = paired(d, 1, 1).astype(jnp.bfloat16)
        send(work.at[d, 1, 1], hop_in.at[d], square_sem.at[0, d], y_next if d % 2 else x_next)
        a, b = (0, 1) if d % 2 else (1, 0)
        work[d, a, b] = paired(d, a, b).astype(jnp.bfloat16)
        send(work.at[d, a, b], direct_in.at[d], square_sem.at[1, d], y_next if d % 2 else x_next)
    for d in order:
        a, b = (1, 0) if d % 2 else (0, 1)
        value = paired(d, a, b)
        arrive(hop_in.at[d], square_sem.at[0, d])
        work[d, a, b] = (value + hop_in[d].astype(jnp.float32)).astype(jnp.bfloat16)
        send(work.at[d, a, b], relay_in.at[d], square_sem.at[2, d], x_next if d % 2 else y_next)
    for d in order:
        value = paired(d, 0, 0)
        arrive(direct_in.at[d], square_sem.at[1, d])
        value = value + direct_in[d].astype(jnp.float32)
        arrive(relay_in.at[d], square_sem.at[2, d])
        value = value + relay_in[d].astype(jnp.float32)
        if d:
            work[d, 0, 0] = value.astype(jnp.bfloat16)
            send(work.at[d, 0, 0], column_in.at[d], column_sem.at[d], columns[d - 1])
        else:
            total = value
    arrive(heads_twin.at[0], heads_sem.at[0])
    arrive(heads_in, heads_sem.at[2])
    projected = (
        heads_ref[y * 2 + core].astype(jnp.float32)
        + heads_twin[0].astype(jnp.float32)
        + heads_in[...].astype(jnp.float32)
    )
    mixed_ref[...] = rms_rows(projected, gain_ref[...]).astype(jnp.bfloat16)
    for d in range(1, depth):
        arrive(column_in.at[d], column_sem.at[d])
        total = total + column_in[d].astype(jnp.float32)
    moe_ref[...] = total.astype(jnp.bfloat16)
    for copy in started:
        copy.wait_send()


def reduce_blocks(part, heads, gain):
    experts, parts, rows, width = part.shape
    depth = experts // 2
    vmem = pl.BlockSpec(memory_space=pltpu.VMEM)
    block = (rows, width)
    held = lambda *lead: pltpu.VMEM(lead + block, jnp.bfloat16)
    sems = lambda *shape: pltpu.SemaphoreType.DMA(shape)
    return pl.pallas_call(
        functools.partial(reduce_kernel, depth),
        out_shape=[jax.ShapeDtypeStruct(block, jnp.bfloat16)] * 2,
        in_specs=[vmem] * 3,
        out_specs=[vmem] * 2,
        scratch_shapes=[
            held(depth, 2, 2), held(depth, 2, 2), held(depth), held(depth), held(depth), held(depth),
            held(), held(2), held(),
            sems(3 + 4 * depth + 3 * depth + depth - 1), sems(depth, 2, 2), sems(3, depth),
            sems(depth), sems(3),
        ],
        compiler_params=pltpu.CompilerParams(
            collective_id=1, has_side_effects=True, vmem_limit_bytes=48 * 1024 * 1024
        ),
        name="reduce_blocks",
    )(part, heads, gain.reshape(1, -1))


def dense_local(
    mix_in, mix_gain, query_weight, latent_weight, rotary_weight, latent_gain, key_weight,
    value_weight, output_weight, out_gain, ffn_in, ffn_gain, gate_weight, up_weight, down_weight,
    routes, route_scores,
):
    f32, bf16 = jnp.float32, jnp.bfloat16
    experts, parts = lax.axis_size("ep"), lax.axis_size("tp")
    ep, tp = lax.axis_index("ep"), lax.axis_index("tp")
    row_count, width = mix_in.shape
    quarter = row_count // parts
    latent_width = latent_weight.shape[1]
    half = ROPE // 2
    first_row = ep * row_count

    def own(array):
        return lax.dynamic_slice_in_dim(array, tp * quarter, quarter, 0)

    rows = rms_rows(own(ffn_in).astype(f32), ffn_gain).astype(bf16)
    own_normed = rms_rows(own(mix_in).astype(f32), mix_gain).astype(bf16)
    latent = rms_rows(jnp.dot(own_normed, latent_weight, preferred_element_type=f32), latent_gain)
    turned = jnp.dot(own_normed, rotary_weight, preferred_element_type=f32)
    positions = first_row + jnp.arange(row_count, dtype=jnp.int32)
    inverse = rope_base ** (-jnp.arange(0, ROPE, 2).astype(f32) / ROPE)
    angles = positions.astype(f32)[:, None] * inverse[None, :]
    cosine, sine = jnp.cos(angles), jnp.sin(angles)

    def rotate(vectors, cosine, sine):
        upper, lower = vectors[..., :half], vectors[..., half:]
        return jnp.concatenate([upper * cosine - lower * sine, lower * cosine + upper * sine], axis=-1)

    rotary_key = rotate(turned, own(cosine), own(sine))
    shares = jax.nn.softmax(own(route_scores), axis=-1)
    named = own(routes)[:, :, None] == jnp.arange(experts, dtype=jnp.int32)[None, None, :]
    table = jnp.sum(jnp.where(named, shares[:, :, None], 0.0), axis=1)
    coarse = lax.reduce_precision(table, 8, 7)
    used = latent_width + ROPE + 2 * experts
    side_width = -(-used // 128) * 128
    side = jnp.concatenate(
        [latent, rotary_key, coarse, table - coarse, jnp.zeros((quarter, side_width - used), f32)],
        axis=1,
    ).astype(bf16)
    all_rows, all_side = gather_blocks(rows, side, experts, parts)
    tokens = experts * row_count
    all_rows = all_rows.reshape(tokens, width)
    all_side = all_side.reshape(tokens, side_width)

    split = latent_width + ROPE
    share_columns = all_side[:, split : split + 2 * experts].astype(f32)
    share_table = share_columns[:, :experts] + share_columns[:, experts:]
    is_mine = (jnp.arange(experts, dtype=jnp.int32) == ep)[None, :]
    share = jnp.sum(jnp.where(is_mine, share_table, 0.0), axis=1, keepdims=True)
    gate_part = jnp.dot(all_rows, gate_weight[0], preferred_element_type=f32)
    up_part = jnp.dot(all_rows, up_weight[0], preferred_element_type=f32)
    hidden = clamped_unit(gate_part, up_part).astype(bf16)
    part = (jnp.dot(hidden, down_weight[0], preferred_element_type=f32) * share).astype(bf16)

    normed = rms_rows(mix_in.astype(f32), mix_gain).astype(bf16)
    head_count = query_weight.shape[1] // (NOPE + ROPE)
    queries = jnp.dot(normed, query_weight, preferred_element_type=f32).reshape(
        row_count, head_count, NOPE + ROPE
    )
    query_plain = queries[..., :NOPE].astype(bf16)
    query_turn = rotate(queries[..., NOPE:], cosine[:, None, :], sine[:, None, :]).astype(bf16)
    all_latent = all_side[:, :latent_width]
    all_turned = all_side[:, latent_width:split]
    across = (((0,), (1,)), ((), ()))
    keys = lax.dot_general(key_weight, all_latent, across, preferred_element_type=f32).astype(bf16)
    values = lax.dot_general(value_weight, all_latent, across, preferred_element_type=f32).astype(bf16)
    keys = keys.reshape(head_count, NOPE, tokens)
    values = values.reshape(head_count, VD, tokens)
    scores = jnp.einsum("ihd,hdj->hij", query_plain, keys, preferred_element_type=f32)
    scores = scores + jnp.einsum("ihd,jd->hij", query_turn, all_turned, preferred_element_type=f32)
    allowed = jnp.arange(tokens, dtype=jnp.int32)[None, :] <= positions[:, None]
    weights = jnp.where(allowed[None], jnp.exp(scores * (NOPE + ROPE) ** (-0.5)), 0.0)
    totals = jnp.sum(weights, axis=-1)
    weighted = jnp.einsum("hij,hdj->hid", weights.astype(bf16), values, preferred_element_type=f32)
    attended = (weighted / totals[..., None]).astype(bf16)
    mixing = output_weight.reshape(head_count, VD, width)
    heads = jnp.einsum("hid,hde->ie", attended, mixing, preferred_element_type=f32).astype(bf16)
    mixed, moe_out = reduce_blocks(
        part.reshape(experts, parts, quarter, width), heads.reshape(parts, quarter, width), out_gain
    )
    return mixed, moe_out


def solution(mesh):
    experts, parts = mesh.shape["ep"], mesh.shape["tp"]

    def body(*args):
        quarter, choose = args[10].shape[0] // parts, args[15].shape[1]
        every_row = 2 * quarter * choose >= quarter * experts
        paired = parts == 4 and experts % 2 == 0 and (experts // 2) & (experts // 2 - 1) == 0
        return (dense_local if every_row and paired else local)(*args)
    placed = (
        P("ep", None),
        P(),
        P(None, "tp"),
        P(),
        P(),
        P(),
        P(None, "tp"),
        P(None, "tp"),
        P("tp", None),
        P(),
        P("ep", None),
        P(),
        P("ep", None, "tp"),
        P("ep", None, "tp"),
        P("ep", "tp", None),
        P("ep", None),
        P("ep", None),
    )
    return jax.shard_map(
        body,
        mesh=mesh,
        in_specs=placed,
        out_specs=(P(("ep", "tp"), None), P(("ep", "tp"), None)),
        check_vma=False,
    )
```

```python
import jax
import jax.numpy as jnp
import functools
from jax import lax
from jax.experimental import pallas as pl
from jax.experimental.pallas import tpu as pltpu
from jax.sharding import PartitionSpec as P

NOPE = 128
ROPE = 64
VD = 128


norm_eps = 1e-06
clamp_limit = 7.0
gate_slope = 1.702
rope_base = 10000.0


def rms_rows(rows_in, scales):
    mean_square = jnp.mean(rows_in * rows_in, axis=-1, keepdims=True)
    return rows_in * lax.rsqrt(mean_square + norm_eps) * scales


def rms_columns(columns, scales):
    mean_square = jnp.mean(columns * columns, axis=0, keepdims=True)
    return columns * lax.rsqrt(mean_square + norm_eps) * scales[:, None]


def turn_table(positions):
    inverse = rope_base ** (-jnp.arange(0, ROPE, 2).astype(jnp.float32) / ROPE)
    angle_rows = inverse[:, None] * positions.astype(jnp.float32)[None, :]
    return (jnp.cos(angle_rows), jnp.sin(angle_rows))


def clamped_unit(gate_part, linear):
    gate_part = jnp.minimum(gate_part, clamp_limit)
    linear = jnp.clip(linear, -clamp_limit, clamp_limit)
    return gate_part * jax.nn.sigmoid(gate_slope * gate_part) * (linear + 1.0)


def keep_state(running):
    return running


def local(
    mix_in,
    mix_gain,
    query_weight,
    latent_weight,
    rotary_weight,
    latent_gain,
    key_weight,
    value_weight,
    output_weight,
    out_gain,
    ffn_in,
    ffn_gain,
    gate_weight,
    up_weight,
    down_weight,
    routes,
    route_scores,
):
    row_count = mix_in.shape[0]
    first_row = lax.axis_index("ep") * row_count
    last_row = first_row + row_count - 1
    positions = first_row + jnp.arange(row_count, dtype=jnp.int32)
    normed = rms_rows(mix_in.astype(jnp.float32), mix_gain).astype(jnp.bfloat16)
    head_count = query_weight.shape[1] // (NOPE + ROPE)
    half_rope = ROPE // 2
    cosine, sine_rows = turn_table(positions)
    queries = jnp.dot(normed, query_weight, preferred_element_type=jnp.float32).reshape(
        row_count, head_count, NOPE + ROPE
    )
    query_plain = queries[..., :NOPE].astype(jnp.bfloat16)
    query_cos = cosine.T[:, None, :]
    query_sin = sine_rows.T[:, None, :]
    query_upper = queries[..., NOPE : NOPE + half_rope]
    query_lower = queries[..., NOPE + half_rope :]
    query_turn = jnp.concatenate(
        [
            query_upper * query_cos - query_lower * query_sin,
            query_lower * query_cos + query_upper * query_sin,
        ],
        axis=-1,
    ).astype(jnp.bfloat16)
    across = (((0,), (1,)), ((), ()))
    latent = rms_columns(
        lax.dot_general(latent_weight, normed, across, preferred_element_type=jnp.float32),
        latent_gain,
    ).astype(jnp.bfloat16)
    rot_raw = lax.dot_general(rotary_weight, normed, across, preferred_element_type=jnp.float32)
    rotary_key = jnp.concatenate(
        [
            rot_raw[:half_rope] * cosine - rot_raw[half_rope:] * sine_rows,
            rot_raw[half_rope:] * cosine + rot_raw[:half_rope] * sine_rows,
        ],
        axis=0,
    ).astype(jnp.bfloat16)
    score_scale = (NOPE + ROPE) ** (-0.5)
    contract_first = (((0,), (0,)), ((), ()))

    def expand(latent_block):
        key_block = lax.dot_general(
            key_weight, latent_block, contract_first, preferred_element_type=jnp.float32
        ).astype(jnp.bfloat16)
        value_block = lax.dot_general(
            value_weight, latent_block, contract_first, preferred_element_type=jnp.float32
        ).astype(jnp.bfloat16)
        return (key_block, value_block)

    def attend(key_block, value_block, turn_block):
        key_count = key_block.shape[1]
        key_block = key_block.reshape(head_count, NOPE, key_count)
        value_block = value_block.reshape(head_count, VD, key_count)
        scores = jnp.einsum(
            "ihd,hdj->hij", query_plain, key_block, preferred_element_type=jnp.float32
        )
        scores = scores + jnp.einsum(
            "ihd,dj->hij", query_turn, turn_block, preferred_element_type=jnp.float32
        )
        key_places = jnp.arange(key_count, dtype=jnp.int32)
        allowed = key_places[None, :] <= positions[:, None]
        weights = jnp.where(allowed[None], jnp.exp(scores * score_scale), 0.0)
        weighted = jnp.einsum(
            "hij,hdj->hid",
            weights.astype(jnp.bfloat16),
            value_block,
            preferred_element_type=jnp.float32,
        )
        return (jnp.sum(weights, axis=-1), weighted)

    initial = (
        jnp.zeros((head_count, row_count), jnp.float32),
        jnp.zeros((head_count, row_count, VD), jnp.float32),
    )
    shard_piece = (
        lax.all_gather(latent, "ep", axis=1, tiled=True),
        lax.all_gather(rotary_key, "ep", axis=1, tiled=True),
    )

    def compute_piece(running):
        key_block, value_block = expand(shard_piece[0])
        return attend(key_block, value_block, shard_piece[1])

    totals, weighted = lax.cond(jnp.int32(0) > last_row, keep_state, compute_piece, initial)
    attended = (weighted / totals[..., None]).astype(jnp.bfloat16)
    mixing = output_weight.reshape(head_count, VD, output_weight.shape[1])
    partial_value = jnp.einsum("hid,hde->ie", attended, mixing, preferred_element_type=jnp.float32)
    projected = lax.psum_scatter(
        lax.optimization_barrier(partial_value.astype(jnp.bfloat16))
        .astype(jnp.float32)
        .astype(jnp.bfloat16),
        "tp",
        scatter_dimension=0,
        tiled=True,
    ).astype(jnp.float32)
    mixed = rms_rows(projected, out_gain).astype(jnp.bfloat16)
    tokens = ffn_in.shape[0]
    part_count = lax.axis_size("tp")
    quarter_rows = tokens // part_count
    experts = lax.axis_size("ep")
    choose = routes.shape[1]
    capacity = max(2, 2 * quarter_rows * choose // experts)
    slot_count = capacity * part_count
    tp_index = lax.axis_index("tp")
    normed_b = rms_rows(ffn_in.astype(jnp.float32), ffn_gain).astype(jnp.bfloat16)
    padded = jnp.concatenate([normed_b, jnp.zeros((1, normed_b.shape[1]), jnp.bfloat16)], axis=0)
    gate_share = jax.nn.softmax(route_scores, axis=-1)
    grouped = routes.reshape(part_count, quarter_rows * choose)
    onehot = (grouped[:, :, None] == jnp.arange(experts, dtype=jnp.int32)[None, None, :]).astype(
        jnp.int32
    )
    slot_rank = jnp.sum((jnp.cumsum(onehot, axis=1) - 1) * onehot, axis=2)
    slot_index = jnp.arange(part_count, dtype=jnp.int32)[:, None] * capacity + slot_rank
    place_index = (slot_index * experts + grouped).reshape(-1)
    owners = jnp.arange(tokens * choose, dtype=jnp.int32) // choose
    slot_token = jnp.full((slot_count * experts,), tokens, jnp.int32).at[place_index].set(owners)
    unit_count = gate_weight.shape[2]
    chosen = lax.dynamic_slice_in_dim(
        slot_token, tp_index * capacity * experts, capacity * experts, 0
    )
    outgoing = padded[chosen].reshape(capacity, experts, -1)
    arrived = lax.all_to_all(outgoing, "ep", split_axis=1, concat_axis=1, tiled=True)
    row_block = lax.all_gather(arrived, "tp", axis=0, tiled=True)
    block_slots = row_block.shape[0]
    flat_rows = row_block.reshape(-1, row_block.shape[2])
    gate_part = jnp.dot(flat_rows, gate_weight[0], preferred_element_type=jnp.float32)
    up_part = jnp.dot(flat_rows, up_weight[0], preferred_element_type=jnp.float32)
    hidden = (
        clamped_unit(gate_part, up_part).astype(jnp.bfloat16).reshape(block_slots, -1, unit_count)
    )
    sources = hidden.shape[1]
    hidden_flat = hidden.reshape(slot_count * sources, unit_count)
    partial_value = jnp.dot(hidden_flat, down_weight[0], preferred_element_type=jnp.float32)
    result = lax.psum_scatter(
        lax.optimization_barrier(partial_value.astype(jnp.bfloat16))
        .astype(jnp.float32)
        .astype(jnp.bfloat16),
        "tp",
        scatter_dimension=0,
        tiled=True,
    )
    result = result.reshape(capacity, sources, -1)
    returned = lax.all_to_all(result, "ep", split_axis=1, concat_axis=1, tiled=True)
    back_rows = returned.reshape(capacity * experts, -1)
    own_rank = lax.dynamic_index_in_dim(slot_rank, tp_index, 0, keepdims=False)
    own_expert = lax.dynamic_index_in_dim(grouped, tp_index, 0, keepdims=False)
    picked = (
        back_rows[own_rank * experts + own_expert]
        .astype(jnp.float32)
        .reshape(quarter_rows, choose, -1)
    )
    own_gates = lax.dynamic_slice_in_dim(gate_share, tp_index * quarter_rows, quarter_rows, 0)
    moe_out = jnp.sum(picked * own_gates[:, :, None], axis=1).astype(jnp.bfloat16)
    return (mixed, moe_out)


MESH = pl.DeviceIdType.MESH


def flip(value, bits):
    bit = 1
    while bit <= bits:
        if bits & bit:
            value = value + bit - 2 * bit * ((value // bit) % 2)
        bit *= 2
    return value


def here():
    ep, tp = lax.axis_index("ep"), lax.axis_index("tp")
    return ep // 2, ep % 2, tp // 2, tp % 2


def place(z, x, y, core):
    return {"ep": z * 2 + x, "tp": y * 2 + core}


def greet(partners):
    barrier = pltpu.get_barrier_semaphore()
    for partner in partners:
        pl.semaphore_signal(barrier, inc=1, device_id=partner, device_id_type=MESH)
    pl.semaphore_wait(barrier, len(partners))


def layer_kernel(
    depth, heads, row_ref, side_ref, query_ref, gain_ref, gate_hbm, up_hbm, down_hbm, key_hbm,
    value_hbm, output_hbm, mixed_ref, moe_ref,
    rows_all, side_all, part_ref, work, twin_in, hop_in, direct_in, relay_in, column_in,
    heads_ref, heads_work, heads_twin, heads_in, keys, values, attended, own_total,
    gate_ref, up_ref, down_ref, key_ref, value_ref, output_ref,
    spread_sem, recv_sem, send_sem, twin_sem, square_sem, column_sem, heads_sem, load_sem,
):
    f32, bf16 = jnp.float32, jnp.bfloat16
    ep = lax.axis_index("ep")
    z, x, y, core = here()
    x_next, y_next, twin = place(z, 1 - x, y, core), place(z, x, 1 - y, core), place(z, x, y, 1 - core)
    columns = [place(flip(z, d), x, y, core) for d in range(1, depth)]
    parts, quarter, width = part_ref.shape[1:]
    row_count = parts * quarter
    side_width = side_ref.shape[1]
    latent_width = key_ref.shape[0]
    experts = 2 * depth
    loads = [
        pltpu.make_async_copy(src, dst, load_sem.at[n])
        for n, (src, dst) in enumerate(
            (
                (gate_hbm, gate_ref), (up_hbm, up_ref), (down_hbm, down_ref),
                (key_hbm, key_ref), (value_hbm, value_ref), (output_hbm, output_ref),
            )
        )
    ]
    for load in loads:
        load.start()
    greet(columns + [x_next, y_next, twin])
    spread, started = [], []

    def copies(origin, target, own):
        e, t = origin["ep"], origin["tp"]
        number = len(spread)
        return [
            pltpu.make_async_remote_copy(
                src_ref=held if own else out.at[e, t],
                dst_ref=out.at[e, t],
                send_sem=spread_sem.at[a, number],
                recv_sem=recv_sem.at[a, e, t],
                device_id=target,
                device_id_type=MESH,
            )
            for a, (held, out) in enumerate(((side_ref, side_all), (row_ref, rows_all)))
        ]

    def give(origin, target, own=False):
        pair = copies(origin, target, own)
        for copy in pair:
            copy.start()
        spread.append(pair)

    def take(origin):
        for copy in copies(origin, twin, False):
            copy.wait_recv()

    def make(src, dst, sem, target):
        return pltpu.make_async_remote_copy(
            src_ref=src, dst_ref=dst, send_sem=send_sem.at[len(started)], recv_sem=sem,
            device_id=target, device_id_type=MESH,
        )

    def send(src, dst, sem, target):
        copy = make(src, dst, sem, target)
        copy.start()
        started.append(copy)

    def arrive(dst, sem):
        make(dst, dst, sem, twin).wait_recv()

    def forward_column(d):
        origin = place(flip(z, d), x, y, core)
        take(origin)
        for target in (x_next, y_next, twin):
            give(origin, target)

    def forward_square(d):
        at = flip(z, d)
        from_x, from_y = place(at, 1 - x, y, core), place(at, x, 1 - y, core)
        take(from_x)
        if d % 2 == 0:
            give(from_x, y_next)
        give(from_x, twin)
        take(from_y)
        if d % 2 == 1:
            give(from_y, x_next)
        give(from_y, twin)

    def forward_corner(d):
        origin = place(flip(z, d), 1 - x, 1 - y, core)
        take(origin)
        give(origin, twin)

    def side_block(e):
        return side_all[e].reshape(row_count, side_width)

    lane = lax.broadcasted_iota(jnp.int32, (row_count, side_width - latent_width), 1)
    is_mine = (lane == ROPE + ep) | (lane == ROPE + experts + ep)

    def expert_plane(d):
        for a in (0, 1):
            for b in (0, 1):
                take(place(flip(z, d), flip(x, a), flip(y, b), 1 - core))

        @pl.loop(0, 2)
        def _(i):
            e = flip(z, d) * 2 + i
            block = rows_all[e].reshape(row_count, width)
            gate_part = jnp.dot(block, gate_ref[...], preferred_element_type=f32)
            up_part = jnp.dot(block, up_ref[...], preferred_element_type=f32)
            hidden = clamped_unit(gate_part, up_part).astype(bf16)
            table = side_block(e)[:, latent_width:].astype(f32)
            share = jnp.sum(jnp.where(is_mine, table, 0.0), axis=1, keepdims=True)
            chunk = 512
            for n in range(0, width, chunk):
                piece = jnp.dot(hidden, down_ref[:, n : n + chunk], preferred_element_type=f32) * share
                part_ref[e, :, :, n : n + chunk] = piece.astype(bf16).reshape(parts, quarter, chunk)

        for a, b in ((1, 1), (1, 0), (0, 1), (0, 0)):
            e, t = flip(z, d) * 2 + flip(x, a), flip(y, b) * 2 + 1 - core
            send(part_ref.at[e, t], twin_in.at[d, a, b], twin_sem.at[d, a, b], twin)

    def paired(d, a, b):
        arrive(twin_in.at[d, a, b], twin_sem.at[d, a, b])
        own = part_ref[flip(z, d) * 2 + flip(x, a), flip(y, b) * 2 + core]
        return own.astype(f32) + twin_in[d, a, b].astype(f32)

    def sum_pairs(d):
        work[d, 1, 1] = paired(d, 1, 1).astype(bf16)
        send(work.at[d, 1, 1], hop_in.at[d], square_sem.at[0, d], y_next if d % 2 else x_next)
        a, b = (0, 1) if d % 2 else (1, 0)
        work[d, a, b] = paired(d, a, b).astype(bf16)
        send(work.at[d, a, b], direct_in.at[d], square_sem.at[1, d], y_next if d % 2 else x_next)

    def sum_relay(d):
        a, b = (1, 0) if d % 2 else (0, 1)
        value = paired(d, a, b)
        arrive(hop_in.at[d], square_sem.at[0, d])
        work[d, a, b] = (value + hop_in[d].astype(f32)).astype(bf16)
        send(work.at[d, a, b], relay_in.at[d], square_sem.at[2, d], x_next if d % 2 else y_next)

    def sum_square(d):
        value = paired(d, 0, 0)
        arrive(direct_in.at[d], square_sem.at[1, d])
        value = value + direct_in[d].astype(f32)
        arrive(relay_in.at[d], square_sem.at[2, d])
        value = value + relay_in[d].astype(f32)
        if d:
            work[d, 0, 0] = value.astype(bf16)
            send(work.at[d, 0, 0], column_in.at[d], column_sem.at[d], columns[d - 1])
        else:
            own_total[...] = value

    across = (((1,), (1,)), ((), ()))
    score_scale = (NOPE + ROPE) ** (-0.5)

    def expand():
        @pl.loop(0, experts)
        def _(e):
            block = side_block(e)
            latent, rest = block[:, :latent_width], block[:, latent_width:]
            at = pl.ds(pl.multiple_of(e * row_count, row_count), row_count)
            key_block = jnp.dot(latent, key_ref[...], preferred_element_type=f32).astype(bf16)
            value_block = jnp.dot(latent, value_ref[...], preferred_element_type=f32).astype(bf16)
            for h in range(heads):
                keys[h, at, :NOPE] = key_block[:, h * NOPE : (h + 1) * NOPE]
                keys[h, at, NOPE:] = rest
                values[h, at, :] = value_block[:, h * VD : (h + 1) * VD]

    def attend(h):
        tokens = experts * row_count
        chunk = 256
        totals = jnp.zeros((row_count, 1), f32)
        weighted = jnp.zeros((row_count, VD), f32)
        places = lax.broadcasted_iota(jnp.int32, (row_count, chunk), 0) + ep * row_count
        for n in range(0, tokens, chunk):
            scores = lax.dot_general(
                query_ref[h], keys[h, n : n + chunk, :], across, preferred_element_type=f32
            )
            allowed = lax.broadcasted_iota(jnp.int32, (row_count, chunk), 1) + n <= places
            weights = jnp.where(allowed, jnp.exp(scores * score_scale), 0.0)
            totals = totals + jnp.sum(weights, axis=1, keepdims=True)
            weighted = weighted + jnp.dot(
                weights.astype(bf16), values[h, n : n + chunk, :], preferred_element_type=f32
            )
        attended[:, h * VD : (h + 1) * VD] = (weighted / totals).astype(bf16)

    def project():
        chunk = 512
        for n in range(0, width, chunk):
            piece = jnp.dot(attended[...], output_ref[:, n : n + chunk], preferred_element_type=f32)
            heads_ref[:, :, n : n + chunk] = piece.astype(bf16).reshape(parts, quarter, chunk)
        for b in (1, 0):
            send(heads_ref.at[flip(y, b) * 2 + 1 - core], heads_twin.at[b], heads_sem.at[b], twin)

    me = place(z, x, y, core)
    for target in columns + [x_next, y_next, twin]:
        give(me, target, True)
    rows_all[me["ep"], me["tp"]] = row_ref[...]
    side_all[me["ep"], me["tp"]] = side_ref[...]
    for load in loads:
        load.wait()

    def reduce_after(last):
        for step, back in ((sum_pairs, 0), (sum_relay, 1), (sum_square, 2)):
            if 0 <= last - back < depth:
                step(last - back)

    for d in range(1, depth + 3):
        if d < depth:
            forward_column(d)
        if d - 1 < depth:
            forward_square(d - 1)
        if 0 <= d - 2 < depth:
            forward_corner(d - 2)
        if 0 <= d - 3 < depth:
            expert_plane(d - 3)
        if 0 <= d - 4:
            reduce_after(d - 4)
    expand()
    reduce_after(depth - 1)
    for h in range(heads):
        attend(h)
        if h % 2 == 0 and h < 4:
            reduce_after(depth + h // 2)
    for h in range((heads + 1) // 2, 2):
        reduce_after(depth + h)
    project()
    arrive(heads_twin.at[1], heads_sem.at[1])
    heads_work[...] = (
        heads_ref[(1 - y) * 2 + core].astype(f32) + heads_twin[1].astype(f32)
    ).astype(bf16)
    send(heads_work, heads_in, heads_sem.at[2], y_next)
    total = own_total[...]
    for d in range(1, depth):
        arrive(column_in.at[d], column_sem.at[d])
        total = total + column_in[d].astype(f32)
    moe_ref[...] = total.astype(bf16)
    arrive(heads_twin.at[0], heads_sem.at[0])
    arrive(heads_in, heads_sem.at[2])
    projected = (
        heads_ref[y * 2 + core].astype(f32) + heads_twin[0].astype(f32) + heads_in[...].astype(f32)
    )
    mixed_ref[...] = rms_rows(projected, gain_ref[...]).astype(bf16)
    for copy in started:
        copy.wait_send()
    for pair in spread:
        for copy in pair:
            copy.wait_send()


def layer(rows, side, queries, gain, weights, experts, parts):
    depth, heads = experts // 2, queries.shape[0]
    quarter, width = rows.shape
    row_count = quarter * parts
    tokens = experts * row_count
    vmem, anywhere = pl.BlockSpec(memory_space=pltpu.VMEM), pl.BlockSpec(memory_space=pl.ANY)
    held = lambda *lead: pltpu.VMEM(lead + (quarter, width), jnp.bfloat16)
    scratch = lambda *shape: pltpu.VMEM(shape, jnp.bfloat16)
    sems = lambda *shape: pltpu.SemaphoreType.DMA(shape)
    gives = depth + 2 + 3 * (depth - 1) + 3 * depth + depth
    return pl.pallas_call(
        functools.partial(layer_kernel, depth, heads),
        out_shape=[jax.ShapeDtypeStruct((quarter, width), jnp.bfloat16)] * 2,
        in_specs=[vmem] * 4 + [anywhere] * len(weights),
        out_specs=[vmem] * 2,
        scratch_shapes=[
            held(experts, parts), scratch(experts, parts, quarter, side.shape[1]),
            held(experts, parts), held(depth, 2, 2), held(depth, 2, 2),
            held(depth), held(depth), held(depth), held(depth),
            held(parts), held(), held(2), held(),
            scratch(heads, tokens, queries.shape[2]), scratch(heads, tokens, VD),
            scratch(row_count, heads * VD), pltpu.VMEM((quarter, width), jnp.float32),
        ]
        + [scratch(*w.shape) for w in weights]
        + [
            sems(2, gives + 1), sems(2, experts, parts), sems(3 + 8 * depth), sems(depth, 2, 2),
            sems(3, depth), sems(depth), sems(3), sems(len(weights)),
        ],
        compiler_params=pltpu.CompilerParams(
            collective_id=0, has_side_effects=True, vmem_limit_bytes=56 * 1024 * 1024
        ),
        name="layer",
    )(rows, side, queries, gain.reshape(1, -1), *weights)


def dense_local(
    mix_in, mix_gain, query_weight, latent_weight, rotary_weight, latent_gain, key_weight,
    value_weight, output_weight, out_gain, ffn_in, ffn_gain, gate_weight, up_weight, down_weight,
    routes, route_scores,
):
    f32, bf16 = jnp.float32, jnp.bfloat16
    experts, parts = lax.axis_size("ep"), lax.axis_size("tp")
    ep, tp = lax.axis_index("ep"), lax.axis_index("tp")
    row_count, width = mix_in.shape
    quarter = row_count // parts
    latent_width = latent_weight.shape[1]
    half = ROPE // 2
    first_row = ep * row_count

    def own(array):
        return lax.dynamic_slice_in_dim(array, tp * quarter, quarter, 0)

    rows = rms_rows(own(ffn_in).astype(f32), ffn_gain).astype(bf16)
    own_normed = rms_rows(own(mix_in).astype(f32), mix_gain).astype(bf16)
    latent = rms_rows(jnp.dot(own_normed, latent_weight, preferred_element_type=f32), latent_gain)
    turned = jnp.dot(own_normed, rotary_weight, preferred_element_type=f32)
    positions = first_row + jnp.arange(row_count, dtype=jnp.int32)
    inverse = rope_base ** (-jnp.arange(0, ROPE, 2).astype(f32) / ROPE)
    angles = positions.astype(f32)[:, None] * inverse[None, :]
    cosine, sine = jnp.cos(angles), jnp.sin(angles)

    def rotate(vectors, cosine, sine):
        upper, lower = vectors[..., :half], vectors[..., half:]
        return jnp.concatenate([upper * cosine - lower * sine, lower * cosine + upper * sine], axis=-1)

    rotary_key = rotate(turned, own(cosine), own(sine))
    shares = jax.nn.softmax(own(route_scores), axis=-1)
    named = own(routes)[:, :, None] == jnp.arange(experts, dtype=jnp.int32)[None, None, :]
    table = jnp.sum(jnp.where(named, shares[:, :, None], 0.0), axis=1)
    coarse = lax.reduce_precision(table, 8, 7)
    used = latent_width + ROPE + 2 * experts
    side_width = -(-used // 128) * 128
    side = jnp.concatenate(
        [latent, rotary_key, coarse, table - coarse, jnp.zeros((quarter, side_width - used), f32)],
        axis=1,
    ).astype(bf16)
    normed = rms_rows(mix_in.astype(f32), mix_gain).astype(bf16)
    head_count = query_weight.shape[1] // (NOPE + ROPE)
    queries = jnp.dot(normed, query_weight, preferred_element_type=f32).reshape(
        row_count, head_count, NOPE + ROPE
    )
    query_turn = rotate(queries[..., NOPE:], cosine[:, None, :], sine[:, None, :])
    spare = jnp.zeros((row_count, head_count, side_width - latent_width - ROPE), f32)
    queries = jnp.concatenate([queries[..., :NOPE], query_turn, spare], axis=-1)
    queries = queries.astype(bf16).transpose(1, 0, 2)
    weights = (
        gate_weight[0], up_weight[0], down_weight[0], key_weight, value_weight, output_weight
    )
    mixed, moe_out = layer(rows, side, queries, out_gain, weights, experts, parts)
    return mixed, moe_out


def solution(mesh):
    experts, parts = mesh.shape["ep"], mesh.shape["tp"]

    def body(*args):
        quarter, choose = args[10].shape[0] // parts, args[15].shape[1]
        every_row = 2 * quarter * choose >= quarter * experts
        paired = parts == 4 and experts % 2 == 0 and (experts // 2) & (experts // 2 - 1) == 0
        return (dense_local if every_row and paired else local)(*args)
    placed = (
        P("ep", None),
        P(),
        P(None, "tp"),
        P(),
        P(),
        P(),
        P(None, "tp"),
        P(None, "tp"),
        P("tp", None),
        P(),
        P("ep", None),
        P(),
        P("ep", None, "tp"),
        P("ep", None, "tp"),
        P("ep", "tp", None),
        P("ep", None),
        P("ep", None),
    )
    return jax.shard_map(
        body,
        mesh=mesh,
        in_specs=placed,
        out_specs=(P(("ep", "tp"), None), P(("ep", "tp"), None)),
        check_vma=False,
    )
```
